32 devices in a mesh: fs: 16 (over z, y, x), tp: 2 (over core).
Axes of the slice: x: 2, y: 2, z: 4, core: 2. Of those that a mesh axis runs over, the one named last changes fastest.
Arguments:
- tokens: bfloat16 [12288, 2048], P('fs'), may hold values from -6 to 6
- norm_gain: float32 [2048], replicated, may hold values from 0.1 to 1.9
- up_weight: float32 [2048, 8192], P('fs', 'tp'), may hold values from -0.125 to 0.125
- up_scale: float32 [8192], P('tp'), may hold values from 0.5 to 2
- down_weight: float32 [8192, 2048], P('tp', 'fs'), may hold values from -0.0625 to 0.0625
- down_scale: float32 [2048], P('fs'), may hold values from 0.5 to 2
Outputs:
- output: bfloat16 [12288, 2048], P('fs', 'tp')
The draws below stay inside these ranges and needn't reach their ends.
All inputs are finite; a program needn't handle non-finite values.
Results may differ from the reference program's by a relative error of at most 0.015.
Values may be sent and summed in bfloat16 or wider, within the bound.
A program may use at most 128 MiB of HBM per device.

```python
import math
import jax
import jax.numpy as jnp
from jax import lax

D = 2048
FF = 8192
TOKENS = 12288
N_TP = 2


def level_of(stream_key, dims, split, least, high):
    def one(axis_at, shards_of):
        steps = jax.random.uniform(jax.random.fold_in(jax.random.fold_in(stream_key, 6), axis_at), (shards_of,), jnp.float32, least / len(split), high / len(split))
        return jnp.repeat(jnp.exp(steps), dims[axis_at] // shards_of).reshape((-1,) + (1,) * (len(dims) - axis_at - 1))

    factor_of = one(*split[0])
    for cut in split[1:]:
        factor_of = factor_of * one(*cut)
    return factor_of


def scatter_about(rng, dims, deviation, most, pieces=(), kind=jnp.bfloat16):
    level = level_of(rng, dims, pieces, -0.22, 0.18) if pieces else 1.0
    drawn = jax.random.normal(rng, dims, jnp.float32) * deviation * level
    return jnp.minimum(jnp.maximum(drawn, -most), most).astype(kind)


def setup_inputs(seed: int = 0) -> dict:
    seeds = jax.random.split(jax.random.key(seed), 7)
    return {
        "tokens": scatter_about(seeds[0], (TOKENS, D), 1.0, 6.0, ((0, 16),)),
        "norm_gain": jnp.clip(1.0 + 0.18 * jax.random.normal(seeds[1], (D,), jnp.float32), 0.1, 1.9),
        "up_weight": scatter_about(seeds[2], (D, FF), D ** -0.5, 0.125, ((0, 16), (1, 2)), jnp.float32),
        "up_scale": jnp.clip(jnp.exp(math.log(2.0) - 1.3862944 * jax.random.uniform(seeds[3], (FF,), jnp.float32) ** level_of(seeds[3], (FF,), ((0, 2),), -0.2, 0.2)), 0.5, 2.0),
        "down_weight": scatter_about(seeds[4], (FF, D), FF ** -0.5, 0.0625, ((0, 2), (1, 16)), jnp.float32),
        "down_scale": jnp.clip(jnp.exp(math.log(2.0) - 1.3862944 * jax.random.uniform(seeds[5], (D,), jnp.float32) ** level_of(seeds[5], (D,), ((0, 16),), -0.2, 0.2)), 0.5, 2.0),
    }


epsilon = 1e-06

def reference(tokens, norm_gain, up_weight, up_scale, down_weight, down_scale):
    floats = tokens.astype(jnp.float32)
    inverse = lax.rsqrt(lax.optimization_barrier(jnp.mean(floats * floats, axis=-1, keepdims=True)) + epsilon)
    normed = (floats * inverse * norm_gain).astype(jnp.bfloat16)
    up_half = up_weight.astype(jnp.bfloat16)
    down_half = down_weight.astype(jnp.bfloat16)
    up_pre = jnp.dot(normed, up_half, preferred_element_type=jnp.float32) * up_scale
    hidden = jnp.square(jax.nn.relu(up_pre)).astype(jnp.bfloat16)
    block_width = FF // N_TP
    summed = jnp.zeros((tokens.shape[0], D), jnp.float32)
    for block in range(N_TP):
        lower = block * block_width
        partial_value = jnp.dot(hidden[:, lower:lower + block_width], down_half[lower:lower + block_width], preferred_element_type=jnp.float32).astype(jnp.bfloat16)
        summed = summed + partial_value.astype(jnp.float32)
    return (summed * down_scale).astype(jnp.bfloat16)
```

```python
import functools

import jax
import jax.numpy as jnp
from jax import lax
from jax.experimental import pallas as pl
from jax.experimental.pallas import tpu as pltpu
from jax.sharding import PartitionSpec as P

epsilon = 1e-06


def normalise(tokens, norm_gain):
    floats = tokens.astype(jnp.float32)
    inverse = lax.rsqrt(jnp.mean(floats * floats, axis=-1, keepdims=True) + epsilon)
    return (floats * inverse * norm_gain).astype(jnp.bfloat16)


def plain(tokens, norm_gain, up_weight, up_scale, down_weight, down_scale):
    normed = normalise(tokens, norm_gain)
    up_whole = lax.all_gather(up_weight.astype(jnp.bfloat16), "fs", axis=0, tiled=True)
    up_pre = jnp.dot(normed, up_whole, preferred_element_type=jnp.float32)
    scaled = (down_weight * down_scale).astype(jnp.bfloat16)
    down_whole = lax.all_gather(scaled, "fs", axis=1, tiled=True)
    hidden = jnp.square(jax.nn.relu(up_pre * up_scale)).astype(jnp.bfloat16)
    partial_value = jnp.dot(hidden, down_whole, preferred_element_type=jnp.float32)
    return lax.psum_scatter(
        partial_value.astype(jnp.bfloat16), "tp", scatter_dimension=1, tiled=True
    )


NX, NY = 2, 2


def kernel(nz, x_ref, s_ref, up_ref, down_ref, out_ref,
           u_buf, d_buf, t_buf, h_buf, ssend, srecv, xsend, xrecv, keep,
           send_sems, recv_sems, local_sems):
    me = lax.axis_index("fs")
    c = lax.axis_index("tp")
    x = lax.rem(me, NX)
    y = lax.rem(me // NX, NY)
    z = me // (NX * NY)
    rows = x_ref.shape[0]
    depth = up_ref.shape[0]
    wide = up_ref.shape[1] // NX
    cols = down_ref.shape[1]
    pair = NX * cols

    def fs_of(zz, yy, xx):
        return (zz * NY + yy) * NX + xx

    def wrap(v):
        return lax.rem(v + 2 * nz, nz)

    target = {
        "z+": {"fs": fs_of(wrap(z + 1), y, x), "tp": c},
        "z-": {"fs": fs_of(wrap(z - 1), y, x), "tp": c},
        "y": {"fs": fs_of(z, 1 - y, x), "tp": c},
        "x": {"fs": fs_of(z, y, 1 - x), "tp": c},
        "c": {"fs": me, "tp": 1 - c},
    }

    local = [
        pltpu.make_async_copy(
            up_ref.at[:, pl.ds(pl.multiple_of(x * wide, wide), wide)],
            u_buf.at[pl.ds(pl.multiple_of(me * depth, depth), depth), :], local_sems.at[0]),
        pltpu.make_async_copy(
            down_ref.at[pl.ds(pl.multiple_of(x * wide, wide), wide), :],
            d_buf.at[me // NX, :, pl.ds(pl.multiple_of(x * cols, cols), cols)], local_sems.at[1]),
    ]
    for copy in local:
        copy.start()

    barrier = pltpu.get_barrier_semaphore()
    for where in target.values():
        pl.semaphore_signal(barrier, inc=1, device_id=where, device_id_type=pl.DeviceIdType.MESH)
    pl.semaphore_wait(barrier, len(target))

    slots, started = {}, []

    def copy_of(key, src, dst, way):
        n = slots.setdefault(key, len(slots))
        return pltpu.make_async_remote_copy(
            src_ref=src, dst_ref=dst, send_sem=send_sems.at[n], recv_sem=recv_sems.at[n],
            device_id=target[way], device_id_type=pl.DeviceIdType.MESH)

    def launch(key, src, dst, way):
        copy = copy_of(key, src, dst, way)
        copy.start()
        started.append(copy)

    def arrive(key, dst, way="x"):
        copy_of(key, dst, dst, way).wait_recv()

    def block(kind, part, dz, dy, half):
        zz, yy = wrap(z + dz), lax.rem(y + dy, NY)
        xx = x if part == "A" else 1 - x
        if kind == "U":
            size = depth if half is None else depth // 2
            at = fs_of(zz, yy, xx) * depth + (0 if half in (None, 0) else size)
            return u_buf.at[pl.ds(pl.multiple_of(at, size), size), :]
        size = wide if half is None else wide // 2
        at = 0 if half in (None, 0) else size
        return d_buf.at[zz * NY + yy, pl.ds(at, size), pl.ds(pl.multiple_of(xx * cols, cols), cols)]

    def send(kind, part, dz, dy, way, half=None):
        ref = block(kind, part, dz, dy, half)
        to = {"z+": ((dz - 1) % nz, dy), "z-": ((dz + 1) % nz, dy), "y": (dz % nz, 1 - dy)}[way]
        launch((kind, part) + to + (half,), ref, ref, way)

    def take(kind, part, dz, dy, half=None):
        arrive((kind, part, dz % nz, dy, half), block(kind, part, dz, dy, half))

    def g1(k):
        for way in ("z+", "z-", "y"):
            send(k, "A", 0, 0, way)

    def g2(k):
        take(k, "B", 0, 0)
        for way in ("y", "z+", "z-"):
            send(k, "B", 0, 0, way)

    def g3(k):
        for dz, way, half in ((-1, "z+", 0), (1, "z-", 1)):
            take(k, "A", dz, 0)
            send(k, "A", dz, 0, way, half)
            send(k, "A", dz, 0, "y")

    def g4(k):
        take(k, "B", 0, 1)
        for way in ("z+", "z-"):
            send(k, "B", 0, 1, way)

    def g5(k):
        for dz, way, half in ((-1, "z+", 0), (1, "z-", 1)):
            take(k, "B", dz, 0)
            send(k, "B", dz, 0, way, half)

    def g6(k):
        take(k, "A", 2, 0, 0)
        take(k, "A", 2, 0, 1)
        send(k, "A", 2, 0, "y")

    def g7(k):
        for dz, way, half in ((-1, "z+", 0), (1, "z-", 1)):
            take(k, "B", dz, 1)
            send(k, "B", dz, 1, way, half)

    launch(("U", "B", 0, 0, None),
           up_ref.at[:, pl.ds(pl.multiple_of((1 - x) * wide, wide), wide)],
           u_buf.at[pl.ds(pl.multiple_of(me * depth, depth), depth), :], "x")
    part_rows = rows // 2
    mine_rows = pl.ds(pl.multiple_of(c * part_rows, part_rows), part_rows)
    other_rows = pl.ds(pl.multiple_of((1 - c) * part_rows, part_rows), part_rows)
    launch(("T", "x"), x_ref.at[mine_rows, :], t_buf.at[mine_rows, :], "x")
    launch(("D", "B", 0, 0, None),
           down_ref.at[pl.ds(pl.multiple_of((1 - x) * wide, wide), wide), :],
           d_buf.at[me // NX, :, pl.ds(pl.multiple_of(x * cols, cols), cols)], "x")

    local[0].wait()
    g1("U")
    g2("U")
    g3("U")
    g4("U")
    g5("U")
    g6("U")
    g7("U")
    local[1].wait()
    g1("D")
    arrive(("T", "x"), t_buf.at[mine_rows, :])
    launch(("T", "c"), t_buf.at[mine_rows, :], t_buf.at[mine_rows, :], "c")
    take("U", "A", 0, 1)
    take("U", "A", -1, 1)
    take("U", "A", 1, 1)
    for half in (0, 1):
        take("U", "B", 2, 0, half)
        take("U", "B", 2, 1, half)
    take("U", "A", 2, 1)
    arrive(("T", "c"), t_buf.at[other_rows, :])

    tile_m, tile_n = 256, min(512, wide)

    def up_part(src, base):
        @pl.loop(0, wide // tile_n)
        def _(j):
            at = pl.ds(pl.multiple_of(j * tile_n, tile_n), tile_n)

            @pl.loop(0, rows // tile_m)
            def _(i):
                r = pl.multiple_of(i * tile_m, tile_m)
                pre = jnp.dot(src[pl.ds(r, tile_m), :], u_buf[:, at],
                              preferred_element_type=jnp.float32)
                act = jnp.square(jnp.maximum(pre * s_ref[:, at], 0.0))
                h_buf[pl.ds(base + r, tile_m), at] = act.astype(jnp.bfloat16)

    up_part(x_ref, 0)
    g2("D")
    g3("D")
    up_part(t_buf, rows)
    g4("D")
    g5("D")
    g6("D")
    g7("D")

    stages = [((z + 1) % 2, 0), ((z + 1) % 2, 1), (z % 2, 0), (z % 2, 1)]

    def owned(n, core):
        q, dy = stages[n]
        return (q + core * (nz // 2)) * NY + lax.rem(y + dy, NY)

    def theirs(n):
        zy = owned(n, 1 - c)

        @pl.loop(0, NX * rows // tile_m)
        def _(i):
            r = pl.ds(pl.multiple_of(i * tile_m, tile_m), tile_m)
            ssend[n, r, :] = jnp.dot(h_buf[r, :], d_buf[zy],
                                     preferred_element_type=jnp.float32).astype(jnp.bfloat16)

        launch(("S", n), ssend.at[n], srecv.at[n], "c")

    def mine(n):
        zy = owned(n, c)
        arrive(("S", n), srecv.at[n])

        def total(i):
            r = pl.ds(pl.multiple_of(i, tile_m), tile_m)
            return jnp.dot(h_buf[r, :], d_buf[zy],
                           preferred_element_type=jnp.float32) + srecv[n, r, :].astype(jnp.float32)

        @pl.loop(0, rows // tile_m)
        def _(i):
            r = pl.multiple_of(i * tile_m, tile_m)
            xsend[n, pl.ds(r, tile_m), :] = total(rows + r).astype(jnp.bfloat16)

        launch(("X", n), xsend.at[n], xrecv.at[n], "x")

        @pl.loop(0, rows // tile_m)
        def _(i):
            r = pl.multiple_of(i * tile_m, tile_m)
            keep[n, pl.ds(r, tile_m), :] = total(r)

    def finish(n):
        arrive(("X", n), xrecv.at[n])
        at = pl.multiple_of((owned(n, c) - c * (nz // 2) * NY) * pair, pair)
        out_ref[:, pl.ds(at, pair)] = (keep[n] + xrecv[n].astype(jnp.float32)).astype(out_ref.dtype)

    theirs(0)
    take("D", "A", 0, 1)
    take("D", "A", -1, 1)
    take("D", "A", 1, 1)
    theirs(1)
    mine(0)
    take("D", "B", 2, 0, 0)
    take("D", "B", 2, 0, 1)
    theirs(2)
    mine(1)
    finish(0)
    take("D", "A", 2, 1)
    take("D", "B", 2, 1, 0)
    take("D", "B", 2, 1, 1)
    theirs(3)
    mine(2)
    mine(3)
    finish(1)
    finish(2)
    finish(3)
    for copy in started:
        copy.wait_send()


def fused(nz, tokens, norm_gain, up_weight, up_scale, down_weight, down_scale):
    rows, width = tokens.shape
    depth, hidden = up_weight.shape
    cols = down_weight.shape[1]
    wide = hidden // NX
    x = lax.rem(lax.axis_index("fs"), NX)
    own_scale = lax.dynamic_slice_in_dim(up_scale, x * wide, wide, 0)[None]
    ways = 2 * (8 + 10) + 2 + 8
    vmem = pl.BlockSpec(memory_space=pltpu.VMEM)
    return pl.pallas_call(
        functools.partial(kernel, nz),
        out_shape=jax.ShapeDtypeStruct((rows, width // 2), jnp.bfloat16),
        in_specs=[vmem] * 4,
        out_specs=vmem,
        scratch_shapes=[
            pltpu.VMEM((width, wide), jnp.bfloat16),
            pltpu.VMEM((nz * NY, wide, NX * cols), jnp.bfloat16),
            pltpu.VMEM((rows, width), jnp.bfloat16),
            pltpu.VMEM((NX * rows, wide), jnp.bfloat16),
            pltpu.VMEM((4, NX * rows, NX * cols), jnp.bfloat16),
            pltpu.VMEM((4, NX * rows, NX * cols), jnp.bfloat16),
            pltpu.VMEM((4, rows, NX * cols), jnp.bfloat16),
            pltpu.VMEM((4, rows, NX * cols), jnp.bfloat16),
            pltpu.VMEM((4, rows, NX * cols), jnp.float32),
            pltpu.SemaphoreType.DMA((ways,)),
            pltpu.SemaphoreType.DMA((ways,)),
            pltpu.SemaphoreType.DMA((2,)),
        ],
        compiler_params=pltpu.CompilerParams(
            collective_id=0, has_side_effects=True, vmem_limit_bytes=60 * 1024 * 1024
        ),
    )(
        normalise(tokens, norm_gain),
        own_scale,
        up_weight.astype(jnp.bfloat16),
        (down_weight * down_scale).astype(jnp.bfloat16),
    )


def solution(mesh):
    in_specs = (P("fs", None), P(), P("fs", "tp"), P("tp", "fs"), P("fs"))
    in_specs = in_specs[:3] + (P("tp"),) + in_specs[3:]
    out_specs = P("fs", "tp")
    nz = mesh.shape["fs"] // (NX * NY)
    local = functools.partial(fused, nz) if nz == 4 and mesh.shape["tp"] == 2 else plain
    return jax.shard_map(local, mesh=mesh, in_specs=in_specs, out_specs=out_specs, check_vma=False)
```

```python
import functools

import jax
import jax.numpy as jnp
from jax import lax
from jax.experimental import pallas as pl
from jax.experimental.pallas import tpu as pltpu
from jax.sharding import PartitionSpec as P

epsilon = 1e-06


def normalise(tokens, norm_gain):
    floats = tokens.astype(jnp.float32)
    inverse = lax.rsqrt(jnp.mean(floats * floats, axis=-1, keepdims=True) + epsilon)
    return (floats * inverse * norm_gain).astype(jnp.bfloat16)


def plain(tokens, norm_gain, up_weight, up_scale, down_weight, down_scale):
    normed = normalise(tokens, norm_gain)
    up_whole = lax.all_gather(up_weight.astype(jnp.bfloat16), "fs", axis=0, tiled=True)
    up_pre = jnp.dot(normed, up_whole, preferred_element_type=jnp.float32)
    scaled = (down_weight * down_scale).astype(jnp.bfloat16)
    down_whole = lax.all_gather(scaled, "fs", axis=1, tiled=True)
    hidden = jnp.square(jax.nn.relu(up_pre * up_scale)).astype(jnp.bfloat16)
    partial_value = jnp.dot(hidden, down_whole, preferred_element_type=jnp.float32)
    return lax.psum_scatter(
        partial_value.astype(jnp.bfloat16), "tp", scatter_dimension=1, tiled=True
    )


NX, NY = 2, 2


def kernel(nz, x_ref, s_ref, up_ref, down_ref, out_ref,
           u_buf, d_buf, t_buf, h_buf, ssend, srecv, xsend, xrecv, keep,
           send_sems, recv_sems, local_sems):
    me = lax.axis_index("fs")
    c = lax.axis_index("tp")
    x = lax.rem(me, NX)
    y = lax.rem(me // NX, NY)
    z = me // (NX * NY)
    rows = x_ref.shape[0]
    depth = up_ref.shape[0]
    wide = up_ref.shape[1] // 2
    cols = down_ref.shape[1]
    pair = NX * cols

    def fs_of(zz, yy, xx):
        return (zz * NY + yy) * NX + xx

    def wrap(v):
        return lax.rem(v + 2 * nz, nz)

    target = {
        **{k: {"fs": fs_of(wrap(z + k), y, x), "tp": c} for k in range(1, nz)},
        "y": {"fs": fs_of(z, 1 - y, x), "tp": c},
        "x": {"fs": fs_of(z, y, 1 - x), "tp": c},
        "c": {"fs": me, "tp": 1 - c},
    }

    side = lax.rem(z, 2)
    peer = {"fs": fs_of(z + 1 - 2 * side, y, x), "tp": c}

    def half_of(k):
        at = pl.multiple_of(lax.rem(z + k, 2) * wide, wide)
        return up_ref.at[:, pl.ds(at, wide)], down_ref.at[pl.ds(at, wide), :]

    own_up = u_buf.at[pl.ds(pl.multiple_of(me * depth, depth), depth), :]
    own_down = d_buf.at[me // NX, :, pl.ds(pl.multiple_of(x * cols, cols), cols)]
    local = [
        pltpu.make_async_copy(half_of(0)[0], own_up, local_sems.at[0]),
        pltpu.make_async_copy(half_of(0)[1], own_down, local_sems.at[1]),
    ]
    for copy in local:
        copy.start()

    barrier = pltpu.get_barrier_semaphore()
    for where in target.values():
        pl.semaphore_signal(barrier, inc=1, device_id=where, device_id_type=pl.DeviceIdType.MESH)
    pl.semaphore_wait(barrier, len(target))

    slots, started = {}, []

    def copy_of(key, src, dst, way):
        n = slots.setdefault(key, len(slots))
        return pltpu.make_async_remote_copy(
            src_ref=src, dst_ref=dst, send_sem=send_sems.at[n], recv_sem=recv_sems.at[n],
            device_id=peer if way == "peer" else target[way], device_id_type=pl.DeviceIdType.MESH)

    def launch(key, src, dst, way):
        copy = copy_of(key, src, dst, way)
        copy.start()
        started.append(copy)

    def arrive(key, dst, way="x"):
        copy_of(key, dst, dst, way).wait_recv()

    def block(kind, dz, px, py, half=None):
        zz, yy = wrap(z + dz), lax.rem(y + py, NY)
        xx = lax.rem(x + px, NX)
        if kind == "U":
            size = depth if half is None else depth // 2
            at = fs_of(zz, yy, xx) * depth + (0 if half in (None, 0) else size)
            return u_buf.at[pl.ds(pl.multiple_of(at, size), size), :]
        size = wide if half is None else wide // 2
        at = 0 if half in (None, 0) else size
        return d_buf.at[zz * NY + yy, pl.ds(at, size), pl.ds(pl.multiple_of(xx * cols, cols), cols)]

    def column(kind, *ways):
        for k in ways:
            src, dst = (half_of(k)[0], own_up) if kind == "U" else (half_of(k)[1], own_down)
            launch((kind, nz - k, 0, 0, None), src, dst, k)

    def take(kind, dz, px, py, half=None):
        arrive((kind, dz, px, py, half), block(kind, dz, px, py, half))

    def share(kind, dz):
        if dz:
            take(kind, dz, 0, 0)
        ref = block(kind, dz, 0, 0)
        launch((kind, dz, 1, 0, None), ref, ref, "x")
        launch((kind, dz, 0, 1, None), ref, ref, "y")

    def cross(kind, dz):
        for px, py, way, half in ((1, 0, "y", 0), (0, 1, "x", 1)):
            take(kind, dz, px, py)
            ref = block(kind, dz, px, py, half)
            launch((kind, dz, 1, 1, half), ref, ref, way)

    def corner(kind, dz):
        take(kind, dz, 1, 1, 0)
        take(kind, dz, 1, 1, 1)

    part_rows = rows // 2
    mine_rows = pl.ds(pl.multiple_of(c * part_rows, part_rows), part_rows)
    other_rows = pl.ds(pl.multiple_of((1 - c) * part_rows, part_rows), part_rows)
    column("U", 1, 3)
    local[0].wait()
    share("U", 0)
    cross("U", 0)
    share("U", 1)
    share("U", 3)
    column("U", 2)
    launch(("T", "x"), x_ref.at[mine_rows, :], t_buf.at[mine_rows, :], "peer")
    cross("U", 1)
    share("U", 2)
    column("D", 1, 3)
    cross("U", 3)
    local[1].wait()
    share("D", 0)
    cross("U", 2)
    arrive(("T", "x"), t_buf.at[mine_rows, :])
    launch(("T", "c"), t_buf.at[mine_rows, :], t_buf.at[mine_rows, :], "c")
    for dz in range(nz):
        corner("U", dz)

    tile_m, tile_n = 256, min(512, wide)

    def up_part(src, base):
        @pl.loop(0, wide // tile_n)
        def _(j):
            at = pl.ds(pl.multiple_of(j * tile_n, tile_n), tile_n)

            @pl.loop(0, rows // tile_m)
            def _(i):
                r = pl.multiple_of(i * tile_m, tile_m)
                pre = jnp.dot(src[pl.ds(r, tile_m), :], u_buf[:, at],
                              preferred_element_type=jnp.float32)
                act = jnp.square(jnp.maximum(pre * s_ref[:, at], 0.0))
                h_buf[pl.ds(base + r, tile_m), at] = act.astype(jnp.bfloat16)

    up_part(x_ref, 0)
    cross("D", 0)
    share("D", 1)
    share("D", 3)
    column("D", 2)
    arrive(("T", "c"), t_buf.at[other_rows, :])
    up_part(t_buf, rows)
    cross("D", 1)
    share("D", 2)
    cross("D", 3)

    stages = [((z + 1) % 2, 0), ((z + 1) % 2, 1), (z % 2, 0), (z % 2, 1)]

    def owned(n, core):
        q, dy = stages[n]
        return (q + core * (nz // 2)) * NY + lax.rem(y + dy, NY)

    def theirs(n):
        zy = owned(n, 1 - c)

        @pl.loop(0, 2 * rows // tile_m)
        def _(i):
            r = pl.ds(pl.multiple_of(i * tile_m, tile_m), tile_m)
            ssend[n, r, :] = jnp.dot(h_buf[r, :], d_buf[zy],
                                     preferred_element_type=jnp.float32).astype(jnp.bfloat16)

        launch(("S", n), ssend.at[n], srecv.at[n], "c")

    def mine(n):
        zy = owned(n, c)
        arrive(("S", n), srecv.at[n])

        def total(i):
            r = pl.ds(pl.multiple_of(i, tile_m), tile_m)
            return jnp.dot(h_buf[r, :], d_buf[zy],
                           preferred_element_type=jnp.float32) + srecv[n, r, :].astype(jnp.float32)

        @pl.loop(0, rows // tile_m)
        def _(i):
            r = pl.multiple_of(i * tile_m, tile_m)
            xsend[n, pl.ds(r, tile_m), :] = total(rows + r).astype(jnp.bfloat16)

        met = (n + 2) % 4
        launch(("X", met), xsend.at[n], xrecv.at[met], "peer")

        @pl.loop(0, rows // tile_m)
        def _(i):
            r = pl.multiple_of(i * tile_m, tile_m)
            keep[n, pl.ds(r, tile_m), :] = total(r)

    def finish(n):
        arrive(("X", n), xrecv.at[n])
        at = pl.multiple_of((owned(n, c) - c * (nz // 2) * NY) * pair, pair)
        out_ref[:, pl.ds(at, pair)] = (keep[n] + xrecv[n].astype(jnp.float32)).astype(out_ref.dtype)

    theirs(0)
    corner("D", 1)
    corner("D", 3)
    theirs(1)
    mine(0)
    cross("D", 2)
    theirs(2)
    mine(1)
    corner("D", 0)
    corner("D", 2)
    theirs(3)
    mine(2)
    mine(3)
    for n in (2, 3, 0, 1):
        finish(n)
    for copy in started:
        copy.wait_send()


def fused(nz, tokens, norm_gain, up_weight, up_scale, down_weight, down_scale):
    rows, width = tokens.shape
    depth, hidden = up_weight.shape
    cols = down_weight.shape[1]
    wide = hidden // 2
    side = lax.rem(lax.axis_index("fs") // (NX * NY), 2)
    own_scale = lax.dynamic_slice_in_dim(up_scale, side * wide, wide, 0)[None]
    ways = 2 * (nz - 1 + 4 * nz) + 2 + 8
    vmem = pl.BlockSpec(memory_space=pltpu.VMEM)
    return pl.pallas_call(
        functools.partial(kernel, nz),
        out_shape=jax.ShapeDtypeStruct((rows, width // 2), jnp.bfloat16),
        in_specs=[vmem] * 4,
        out_specs=vmem,
        scratch_shapes=[
            pltpu.VMEM((width, wide), jnp.bfloat16),
            pltpu.VMEM((nz * NY, wide, NX * cols), jnp.bfloat16),
            pltpu.VMEM((rows, width), jnp.bfloat16),
            pltpu.VMEM((2 * rows, wide), jnp.bfloat16),
            pltpu.VMEM((4, 2 * rows, NX * cols), jnp.bfloat16),
            pltpu.VMEM((4, 2 * rows, NX * cols), jnp.bfloat16),
            pltpu.VMEM((4, rows, NX * cols), jnp.bfloat16),
            pltpu.VMEM((4, rows, NX * cols), jnp.bfloat16),
            pltpu.VMEM((4, rows, NX * cols), jnp.float32),
            pltpu.SemaphoreType.DMA((ways,)),
            pltpu.SemaphoreType.DMA((ways,)),
            pltpu.SemaphoreType.DMA((2,)),
        ],
        compiler_params=pltpu.CompilerParams(
            collective_id=0, has_side_effects=True, vmem_limit_bytes=60 * 1024 * 1024
        ),
    )(
        normalise(tokens, norm_gain),
        own_scale,
        up_weight.astype(jnp.bfloat16),
        (down_weight * down_scale).astype(jnp.bfloat16),
    )


def solution(mesh):
    in_specs = (P("fs", None), P(), P("fs", "tp"), P("tp", "fs"), P("fs"))
    in_specs = in_specs[:3] + (P("tp"),) + in_specs[3:]
    out_specs = P("fs", "tp")
    nz = mesh.shape["fs"] // (NX * NY)
    local = functools.partial(fused, nz) if nz == 4 and mesh.shape["tp"] == 2 else plain
    return jax.shard_map(local, mesh=mesh, in_specs=in_specs, out_specs=out_specs, check_vma=False)
```
